512 devices in a mesh: sp: 64 (over z, y), tp: 8 (over x, core).
Axes of the slice: x: 4, y: 4, z: 16, core: 2. Of those that a mesh axis runs over, the one named last changes fastest.
Arguments:
- tokens: bfloat16 [8192, 2048], P('sp', 'tp'), may hold values from -6 to 6
- norm_gain: float32 [2048], replicated, may hold values from 0.1 to 1.9
- w_value: bfloat16 [2048, 2048], P('sp', 'tp'), may hold values from -0.125 to 0.125
- w_gate: bfloat16 [2048, 2048], P('sp', 'tp'), may hold values from -0.125 to 0.125
- conv_taps: bfloat16 [31, 2048], P(None, 'tp'), may hold values from -1 to 1
- conv_gain: float32 [2048], P('tp'), may hold values from 0.1 to 1.9
- w_query: bfloat16 [2048, 3072], P(None, 'tp'), may hold values from -5.303301 to 5.303301
- latent_down_weight: bfloat16 [2048, 512], P('sp'), may hold values from -0.125 to 0.125
- latent_norm_gain: float32 [512], replicated, may hold values from 0.1 to 1.9
- w_rope_key: bfloat16 [2048, 64], P('sp'), may hold values from -0.125 to 0.125
- key_up_weight: bfloat16 [512, 2048], P(None, 'tp'), may hold values from -0.5 to 0.5
- value_up_weight: bfloat16 [512, 2048], P(None, 'tp'), may hold values from -0.25 to 0.25
- w_merge_conv: bfloat16 [2048, 2048], P('tp'), may hold values from -0.09375 to 0.09375
- w_merge_attn: bfloat16 [2048, 2048], P('tp'), may hold values from -0.28125 to 0.28125
Outputs:
- merged: bfloat16 [8192, 2048], P(('sp', 'tp'))
- log_sums: float32 [8192, 16], P('sp', 'tp')
The draws below stay inside these ranges and needn't reach their ends.
All inputs are finite; a program needn't handle non-finite values.
Results may differ from the reference program's by a relative error of at most 0.025.
The reference program's roundings to bfloat16 on the way count: a program that leaves them out, or rounds other values in their place, can miss the bound.
Values may be sent and summed in bfloat16 or wider, within the bound.
A program may use at most 64 MiB of HBM per device.

```python
import jax
import jax.numpy as jnp
from jax import lax

MODEL_WIDTH = 2048
CC = 2048
HEAD_TOTAL = 16
KEY_VALUE_RANK = 512
PLAIN_QK_WIDTH = 128
QK_ROPE = 64
VALUE_HEAD_WIDTH = 128
CONV_WIDTH = 31
TOKEN_TOTAL = 8192
N_TP = 8


def draw_w_query(key, part):
    values = jnp.clip(jax.random.normal(key, (MODEL_WIDTH, HEAD_TOTAL * (PLAIN_QK_WIDTH + QK_ROPE)), jnp.float32), -6.0, 6.0) * MODEL_WIDTH ** (-0.5)
    return values.astype(jnp.bfloat16)


def block_scale(rng, shape, split, smallest, largest):
    level, own = 1.0, jax.random.fold_in(rng, 6)
    for axis_at, blocks in split:
        heights = jnp.exp(jax.random.uniform(jax.random.fold_in(own, axis_at), (blocks,), jnp.float32, smallest / len(split), largest / len(split)))
        level = level * jnp.repeat(heights, shape[axis_at] // blocks).reshape([-1 if axis == axis_at else 1 for axis in range(len(shape))])
    return level


def normal_values(own_key, extent, scale, limit, pieces=(), held_as=jnp.bfloat16):
    array = scale * jax.random.normal(own_key, extent, jnp.float32)
    if pieces:
        array = array * block_scale(own_key, extent, pieces, -0.22, 0.18)
    return jnp.clip(array, -limit, limit).astype(held_as)


def setup_inputs(seed: int = 0) -> dict:
    seeds = jax.random.split(jax.random.key(seed), 15)
    return {
        "tokens": normal_values(seeds[0], (TOKEN_TOTAL, MODEL_WIDTH), 1.0, 6.0, ((0, 64), (1, 8))),
        "norm_gain": jnp.clip(1.0 + 0.18 * jax.random.normal(seeds[1], (MODEL_WIDTH,), jnp.float32), 0.1, 1.9),
        "w_value": normal_values(seeds[2], (MODEL_WIDTH, CC), MODEL_WIDTH ** -0.5, 0.125, ((0, 64), (1, 8))),
        "w_gate": normal_values(seeds[3], (MODEL_WIDTH, CC), MODEL_WIDTH ** -0.5, 0.125, ((0, 64), (1, 8))),
        "conv_taps": normal_values(seeds[4], (CONV_WIDTH, CC), CONV_WIDTH ** -0.5, 1.0, ((1, 8),)),
        "conv_gain": jnp.clip(1.0 + 0.18 * jax.random.normal(seeds[5], (CC,), jnp.float32), 0.1, 1.9),
        "w_query": draw_w_query(jax.random.fold_in(seeds[14], 71), 0),
        "latent_down_weight": normal_values(seeds[7], (MODEL_WIDTH, KEY_VALUE_RANK), MODEL_WIDTH ** -0.5, 0.125, ((0, 64),)),
        "latent_norm_gain": jnp.clip(1.0 + 0.18 * jax.random.normal(seeds[8], (KEY_VALUE_RANK,), jnp.float32), 0.1, 1.9),
        "w_rope_key": normal_values(seeds[9], (MODEL_WIDTH, QK_ROPE), MODEL_WIDTH ** -0.5, 0.125, ((0, 64),)),
        "key_up_weight": normal_values(seeds[10], (KEY_VALUE_RANK, HEAD_TOTAL * PLAIN_QK_WIDTH), PLAIN_QK_WIDTH ** -0.5, 0.5, ((1, 8),)),
        "value_up_weight": normal_values(seeds[11], (KEY_VALUE_RANK, HEAD_TOTAL * VALUE_HEAD_WIDTH), KEY_VALUE_RANK ** -0.5, 0.25, ((1, 8),)),
        "w_merge_conv": normal_values(seeds[12], (CC, MODEL_WIDTH), (CC + HEAD_TOTAL * VALUE_HEAD_WIDTH) ** -0.5, 0.09375, ((0, 8),)),
        "w_merge_attn": normal_values(seeds[13], (HEAD_TOTAL * VALUE_HEAD_WIDTH, MODEL_WIDTH), (3.0 / (CC + HEAD_TOTAL * VALUE_HEAD_WIDTH) ** 0.5), 0.28125, ((0, 8),)),
    }


epsilon = 1e-06
rope_base = 10000.0
masked_score = -1e+30

def angles_at(positions, width):
    inverse = rope_base ** (-2.0 * jnp.arange(width // 2, dtype=jnp.float32) / width)
    return positions[:, None] * inverse[None, :]

def rotate(halves, angle):
    middle = halves.shape[-1] // 2
    first, second = (halves[..., :middle], halves[..., middle:])
    cosine, sine = (jnp.cos(angle), jnp.sin(angle))
    return jnp.concatenate([first * cosine - second * sine, first * sine + second * cosine], axis=-1)

def reference(tokens, norm_gain, w_value, w_gate, conv_taps, conv_gain, w_query, latent_down_weight, latent_norm_gain, w_rope_key, key_up_weight, value_up_weight, w_merge_conv, w_merge_attn):
    features = tokens.astype(jnp.float32)
    normed = (features * lax.rsqrt(lax.optimization_barrier(jnp.mean(features * features, axis=-1, keepdims=True)) + epsilon) * norm_gain).astype(jnp.bfloat16)
    value_pre = jnp.dot(normed, w_value, preferred_element_type=jnp.float32)
    gate_pre = jnp.dot(normed, w_gate, preferred_element_type=jnp.float32)
    gated_rows = (value_pre * jax.nn.sigmoid(gate_pre)).astype(jnp.bfloat16)
    conv_reach = CONV_WIDTH - 1
    padded = jnp.concatenate([jnp.zeros((conv_reach, CC), jnp.bfloat16), gated_rows], axis=0).astype(jnp.float32)
    mixed = jnp.zeros((TOKEN_TOTAL, CC), jnp.float32)
    for tap_index in range(CONV_WIDTH):
        mixed = mixed + conv_taps[tap_index].astype(jnp.float32) * padded[tap_index:tap_index + TOKEN_TOTAL]
    channel_mean = lax.optimization_barrier(jnp.mean(mixed, axis=-1, keepdims=True))
    channel_var = lax.optimization_barrier(jnp.mean(jnp.square(mixed - channel_mean), axis=-1, keepdims=True))
    conv_out = jax.nn.silu((mixed - channel_mean) * lax.rsqrt(channel_var + epsilon) * conv_gain).astype(jnp.bfloat16)
    positions = jnp.arange(TOKEN_TOTAL, dtype=jnp.float32)
    rope_angles = angles_at(positions, QK_ROPE)
    query = jnp.dot(normed, w_query, preferred_element_type=jnp.float32).astype(jnp.bfloat16).reshape(TOKEN_TOTAL, HEAD_TOTAL, PLAIN_QK_WIDTH + QK_ROPE)
    query_rope = rotate(query[..., PLAIN_QK_WIDTH:].astype(jnp.float32), rope_angles[:, None, :]).astype(jnp.bfloat16)
    key_expanded = key_up_weight.astype(jnp.float32).reshape(KEY_VALUE_RANK, HEAD_TOTAL, PLAIN_QK_WIDTH)
    query_latent = jnp.einsum('thd,lhd->thl', query[..., :PLAIN_QK_WIDTH].astype(jnp.float32), key_expanded).astype(jnp.bfloat16)
    latent_pre = jnp.dot(normed, latent_down_weight, preferred_element_type=jnp.float32)
    latent = (latent_pre * lax.rsqrt(lax.optimization_barrier(jnp.mean(latent_pre * latent_pre, axis=-1, keepdims=True)) + epsilon) * latent_norm_gain).astype(jnp.bfloat16)
    key_rope = rotate(jnp.dot(normed, w_rope_key, preferred_element_type=jnp.float32), rope_angles).astype(jnp.bfloat16)
    score_scale = (PLAIN_QK_WIDTH + QK_ROPE) ** (-0.5)
    query_block = min(512, TOKEN_TOTAL)
    key_index = jnp.arange(TOKEN_TOTAL, dtype=jnp.int32)
    latent_wide = latent.astype(jnp.float32)
    rope_wide = key_rope.astype(jnp.float32)

    def one_block(block_start):
        block_latent = lax.dynamic_slice_in_dim(query_latent, block_start, query_block, 0).astype(jnp.float32)
        block_rope = lax.dynamic_slice_in_dim(query_rope, block_start, query_block, 0).astype(jnp.float32)
        scores = (jnp.einsum('thl,kl->thk', block_latent, latent_wide) + jnp.einsum('thr,kr->thk', block_rope, rope_wide)) * score_scale
        query_index = block_start + jnp.arange(query_block, dtype=jnp.int32)
        allowed = key_index[None, None, :] <= query_index[:, None, None]
        scores = jnp.where(allowed, scores, masked_score)
        row_max = lax.optimization_barrier(jnp.max(scores, axis=-1))
        weights = jnp.where(allowed, jnp.exp(scores - row_max[..., None]), 0.0)
        weight_sum = lax.optimization_barrier(jnp.sum(weights, axis=-1))
        weighted = jnp.einsum('thk,kl->thl', weights.astype(jnp.bfloat16).astype(jnp.float32), latent_wide)
        return ((weighted / weight_sum[..., None]).astype(jnp.bfloat16), row_max + jnp.log(weight_sum))
    block_starts = jnp.arange(TOKEN_TOTAL // query_block, dtype=jnp.int32) * query_block
    latent_result, log_sums = lax.map(one_block, block_starts)
    latent_result = latent_result.reshape(TOKEN_TOTAL, HEAD_TOTAL, KEY_VALUE_RANK)
    log_sums = log_sums.reshape(TOKEN_TOTAL, HEAD_TOTAL)
    value_expanded = value_up_weight.astype(jnp.float32).reshape(KEY_VALUE_RANK, HEAD_TOTAL, VALUE_HEAD_WIDTH)
    attention = jnp.einsum('thl,lhv->thv', latent_result.astype(jnp.float32), value_expanded).astype(jnp.bfloat16).reshape(TOKEN_TOTAL, HEAD_TOTAL * VALUE_HEAD_WIDTH)
    channel_share = CC // N_TP
    head_share = HEAD_TOTAL * VALUE_HEAD_WIDTH // N_TP
    merged = jnp.zeros((TOKEN_TOTAL, MODEL_WIDTH), jnp.float32)
    for group_index in range(N_TP):
        channel_part = conv_out[:, group_index * channel_share:(group_index + 1) * channel_share]
        head_part = attention[:, group_index * head_share:(group_index + 1) * head_share]
        partial_value = jnp.dot(channel_part, w_merge_conv[group_index * channel_share:(group_index + 1) * channel_share], preferred_element_type=jnp.float32)
        partial_value = partial_value + jnp.dot(head_part, w_merge_attn[group_index * head_share:(group_index + 1) * head_share], preferred_element_type=jnp.float32)
        merged = merged + partial_value.astype(jnp.bfloat16).astype(jnp.float32)
    return (merged.astype(jnp.bfloat16), log_sums)
```

```python
import functools

import jax
import jax.numpy as jnp
from jax import lax
from jax.experimental import pallas as pl
from jax.experimental.pallas import tpu as pltpu
from jax.sharding import Mesh
from jax.sharding import PartitionSpec as P

PLAIN_QK_WIDTH = 128
QK_ROPE = 64
VALUE_HEAD_WIDTH = 128
epsilon = 1e-06
rope_base = 10000.0
masked_score = -1e30
SP = ("z", "y")
TP = ("x", "c")
LANES = 128
VMEM = pl.BlockSpec(memory_space=pltpu.VMEM)
MIB = 1 << 20


class Net:
    def __init__(self, sizes, send, recv):
        self.nz, self.ny, self.nx, self.nc = sizes
        self.z, self.y, self.x, self.c = (lax.axis_index(a) for a in ("z", "y", "x", "c"))
        self.send, self.recv = send, recv
        self.ids, self.open = {}, []

    def number(self, name):
        return self.ids.setdefault(name, len(self.ids))

    def put(self, name, src, dst, **to):
        k = self.number(name)
        copy = pltpu.make_async_remote_copy(
            src_ref=src,
            dst_ref=dst,
            send_sem=self.send.at[k],
            recv_sem=self.recv.at[k],
            device_id=to,
            device_id_type=pl.DeviceIdType.MESH,
        )
        copy.start()
        self.open.append(copy)

    def got(self, name, dst, **to):
        k = self.number(name)
        pltpu.make_async_remote_copy(
            src_ref=dst,
            dst_ref=dst,
            send_sem=self.send.at[k],
            recv_sem=self.recv.at[k],
            device_id=to,
            device_id_type=pl.DeviceIdType.MESH,
        ).wait_recv()

    def finish(self):
        for copy in self.open:
            copy.wait_send()

    def zp(self, d):
        return lax.rem(self.z + d + self.nz, self.nz)

    def yp(self, d):
        return lax.rem(self.y + d + self.ny, self.ny)

    def xp(self, d):
        return lax.rem(self.x + d + self.nx, self.nx)

    def cp(self):
        return 1 - self.c

    def greet(self, peers):
        barrier = pltpu.get_barrier_semaphore()
        for to in peers:
            pl.semaphore_signal(barrier, inc=1, device_id=to, device_id_type=pl.DeviceIdType.MESH)
        pl.semaphore_wait(barrier, len(peers))


def z_plan(nz):
    group = 4 if nz >= 16 else 2
    count = nz // group
    if group == 4:
        near = {1: range(count), -1: range(count), 2: (0, 1), -2: (1, 2)}
    else:
        near = {1: range(count)}
    return group, count, near


def z_peers(net):
    group, count, near = z_plan(net.nz)
    far = (1, -1) if count > 2 else (1,) if count == 2 else ()
    offsets = [group * f for f in far]
    for d in near:
        offsets.append(d)
    peers = [{"z": net.zp(d)} for d in offsets]
    if group == 2:
        peers.append({"z": net.zp(-1)})
    return peers


class ZGather:
    def __init__(self, net, tag, slot):
        self.net, self.tag, self.slot = net, tag, slot
        self.group, self.count, self.near = z_plan(net.nz)
        z_class = net.z // self.group
        self.turn = jnp.where(lax.rem(z_class, 2) == 1, 1, -1)

    def block(self, b):
        return self.slot(self.net.zp(b * self.group))

    def start(self):
        n, g = self.net, self.group
        own = self.block(0)
        if self.count >= 2:
            n.put((self.tag, "f", 1), own, own, z=n.zp(g))
        if self.count > 2:
            n.put((self.tag, "f", -1), own, own, z=n.zp(-g))
        self.spread(0)

    def spread(self, b):
        n = self.net
        for d, blocks in self.near.items():
            if b in blocks:
                n.put((self.tag, "n", d, b), self.block(b), self.block(b), z=n.zp(d))

    def far(self):
        n, g = self.net, self.group
        if self.count == 2:
            n.got((self.tag, "f", 1), self.block(1), z=n.zp(g))
            self.spread(1)
            yield g
            return
        n.got((self.tag, "f", 1), self.block(3), z=n.zp(g))
        n.got((self.tag, "f", -1), self.block(1), z=n.zp(g))
        onward = self.slot(n.zp(-g * self.turn))
        n.put((self.tag, "r"), onward, onward, z=n.zp(g * self.turn))
        self.spread(1)
        self.spread(3)
        yield g
        yield 3 * g
        n.got((self.tag, "r"), self.block(2), z=n.zp(g))
        self.spread(2)
        yield 2 * g

    def close(self):
        n, g = self.net, self.group
        order = (0, 1, 3, 2) if self.count == 4 else range(self.count)
        for b in order:
            for d, blocks in self.near.items():
                if b in blocks:
                    at = (b * g - d) % n.nz
                    n.got((self.tag, "n", d, b), self.slot(n.zp(at)), z=n.zp(d))
                    yield at


def tile(i, size):
    return pl.ds(pl.multiple_of(i * size, size), size)


def gather_inputs(sizes, tok, lw, vg, X, WL, VG, yb, send, recv):
    net = Net(sizes, send, recv)
    nz, ny, nx, nc = sizes
    z, y, x, c = net.z, net.y, net.x, net.c
    half = tok.shape[1] // 2
    wr = lw.shape[0]
    kept = WL.shape[0]

    peers = [{"y": net.yp(k)} for k in range(1, ny)] + [{"x": net.xp(k)} for k in range(1, nx)]
    peers += [{"c": net.cp()}] + z_peers(net)
    net.greet(peers)

    def cols(side, xx, cc):
        return tile((xx * nc + cc) * 2 + side, half)

    def place(side, yy, xx, cc):
        return X.at[yy, :, cols(side, xx, cc)]

    mine = [tok.at[:, pl.ds(0, half)], tok.at[:, pl.ds(half, half)]]
    for k in range(1, ny):
        net.put(("lw", k), lw, yb.at[y], y=net.yp(k))
    for k in range(1, ny):
        net.put(("ya", k), mine[0], place(0, y, x, c), y=net.yp(k))
    for k in range(1, nx):
        net.put(("xb", k), mine[1], place(1, y, x, c), x=net.xp(k))
    for k in range(1, nx):
        net.put(("xa", 0, k), mine[0], place(0, y, x, c), x=net.xp(k))
    for k in range(1, ny):
        net.put(("yb", 0, k), mine[1], place(1, y, x, c), y=net.yp(k))
    for k in range(1, ny):
        net.put(("vg", k), vg.at[net.yp(k)], VG.at[tile(y, wr)], y=net.yp(k))
    for side in (0, 1):
        net.put(("s", side), mine[side], place(side, y, x, c), c=net.cp())
        X[pl.ds(y, 1), :, cols(side, x, c)] = tok[:, side * half : (side + 1) * half][None]
    yb[pl.ds(y, 1)] = lw[...][None]
    VG[tile(y, wr)] = vg[pl.ds(y, 1)].reshape(vg.shape[1:])

    for k in range(1, ny):
        net.got(("lw", k), yb.at[net.yp(-k)], y=net.yp(k))
    rows = yb[...].reshape(ny * wr, yb.shape[2])
    WL[:, tile(z, LANES)] = rows.astype(jnp.float32).T[:kept].astype(WL.dtype)
    zg = ZGather(net, "wl", lambda at: WL.at[:, tile(at, LANES)])
    zg.start()

    for k in range(1, ny):
        here = place(0, net.yp(-k), x, c)
        net.got(("ya", k), here, y=net.yp(k))
        for j in range(1, nx):
            net.put(("xa", k, j), here, here, x=net.xp(j))
        net.put(("sa", k), here, here, c=net.cp())
    for k in range(1, nx):
        here = place(1, y, net.xp(-k), c)
        net.got(("xb", k), here, x=net.xp(k))
        for j in range(1, ny):
            net.put(("yb", k, j), here, here, y=net.yp(j))
        net.put(("sb", k), here, here, c=net.cp())
    for _ in zg.far():
        pass
    for k in range(ny):
        for j in range(1, nx):
            here = place(0, net.yp(-k), net.xp(-j), c)
            net.got(("xa", k, j), here, x=net.xp(j))
            net.put(("sxa", k, j), here, here, c=net.cp())
    for k in range(nx):
        for j in range(1, ny):
            here = place(1, net.yp(-j), net.xp(-k), c)
            net.got(("yb", k, j), here, y=net.yp(j))
            net.put(("syb", k, j), here, here, c=net.cp())
    for _ in zg.close():
        pass
    for k in range(1, ny):
        net.got(("vg", k), VG.at[tile(net.yp(-k), wr)], y=net.yp(k))
    o = net.cp()
    for side in (0, 1):
        net.got(("s", side), place(side, y, x, o), c=o)
    for k in range(1, ny):
        net.got(("sa", k), place(0, net.yp(-k), x, o), c=o)
    for k in range(1, nx):
        net.got(("sb", k), place(1, y, net.xp(-k), o), c=o)
    for k in range(ny):
        for j in range(1, nx):
            net.got(("sxa", k, j), place(0, net.yp(-k), net.xp(-j), o), c=o)
    for k in range(nx):
        for j in range(1, ny):
            net.got(("syb", k, j), place(1, net.yp(-j), net.xp(-k), o), c=o)
    net.finish()


def gather_latent(sizes, own, vg, K, W, send, recv):
    net = Net(sizes, send, recv)
    nz, ny, nx, nc = sizes
    z, x, c = net.z, net.x, net.c
    depth = vg.shape[0]

    peers = [{"x": net.xp(k)} for k in range(1, nx)] + [{"c": net.cp()}] + z_peers(net)
    net.greet(peers)

    def slot(at, xx=None, cc=None):
        j = (x if xx is None else xx) * nc + (c if cc is None else cc)
        return K.at[j, :, tile(at, own.shape[1])]

    K[pl.ds(x * nc + c, 1), :, tile(z, own.shape[1])] = own[...][None]
    W[tile(z, depth)] = vg[...]
    zl = ZGather(net, "l", slot)
    zw = ZGather(net, "w", lambda at: W.at[tile(at, depth)])

    def onward(n):
        here = slot(net.zp(n))
        for k in range(1, nx):
            net.put(("x", n, k), here, here, x=net.xp(k))
        net.put(("s", n), here, here, c=net.cp())

    zl.start()
    onward(0)
    zw.start()
    for n in zl.far():
        onward(n)
    for _ in zw.far():
        pass
    order = [0] + [zl.group * b for b in ((1, 3, 2) if zl.count == 4 else range(1, zl.count))]
    for n in zl.close():
        onward(n)
        order.append(n)
    for n in order:
        for k in range(1, nx):
            here = slot(net.zp(n), net.xp(-k))
            net.got(("x", n, k), here, x=net.xp(k))
            net.put(("sx", n, k), here, here, c=net.cp())
    for _ in zw.close():
        pass
    o = net.cp()
    for n in order:
        net.got(("s", n), slot(net.zp(n), None, o), c=o)
        for k in range(1, nx):
            net.got(("sx", n, k), slot(net.zp(n), net.xp(-k), o), c=o)
    net.finish()


def exchange(sizes, att, mixed, st, att_r, mixed_r, st_r, stat_r, send, recv):
    net = Net(sizes, send, recv)
    nz, ny, nx, nc = sizes
    y, x, c = net.y, net.x, net.c
    rows = att_r.shape[2]
    offsets = [(a, b) for a in range(nx) for b in range(nc) if a or b]

    def there(a, b):
        return {"x": net.xp(a), "c": net.c if b == 0 else net.cp()}

    net.greet([{"y": net.yp(k)} for k in range(1, ny)] + [there(a, b) for a, b in offsets])
    for k in range(1, ny):
        t = net.yp(k)
        net.put(("st", k), st.at[t], st_r.at[y], y=t)
    for k in range(1, ny):
        t = net.yp(k)
        net.put(("m", k), mixed.at[t], mixed_r.at[y], y=t)
        net.put(("a", k), att.at[:, tile(t, rows), :], att_r.at[y], y=t)
    att_r[pl.ds(y, 1)] = att[:, tile(y, rows), :][None]
    mixed_r[pl.ds(y, 1)] = mixed[pl.ds(y, 1)]
    st_r[pl.ds(y, 1)] = st[pl.ds(y, 1)]
    for k in range(1, ny):
        net.got(("st", k), st_r.at[net.yp(-k)], y=net.yp(k))
    me = x * nc + c
    stat_r[pl.ds(me, 1)] = jnp.sum(st_r[...], axis=0)[None]
    for a, b in offsets:
        net.put(("t", a, b), stat_r.at[me], stat_r.at[me], **there(a, b))
    for k in range(1, ny):
        net.got(("m", k), mixed_r.at[net.yp(-k)], y=net.yp(k))
        net.got(("a", k), att_r.at[net.yp(-k)], y=net.yp(k))
    for a, b in offsets:
        j = net.xp(-a) * nc + (net.c if b == 0 else net.cp())
        net.got(("t", a, b), stat_r.at[j], **there(a, b))
    net.finish()


def scatter_rows(sizes, part, out, send, recv):
    net = Net(sizes, send, recv)
    nz, ny, nx, nc = sizes
    x, c = net.x, net.c
    me = x * nc + c
    offsets = [(a, b) for a in range(nx) for b in range(nc) if a or b]

    def there(a, b):
        return {"x": net.xp(a), "c": net.c if b == 0 else net.cp()}

    def index(to):
        return to["x"] * nc + to["c"]

    net.greet([there(a, b) for a, b in offsets])
    for a, b in offsets:
        to = there(a, b)
        net.put((a, b), part.at[index(to)], out.at[me], **to)
    out[pl.ds(me, 1)] = part[pl.ds(me, 1)]
    for a, b in offsets:
        source = there(-a, b)
        net.got((a, b), out.at[index(source)], **there(a, b))
    net.finish()


def kernel_call(body, sizes, outs, messages, cid, args, scratch=(), limit=24 * MIB):
    return pl.pallas_call(
        functools.partial(body, sizes),
        out_shape=outs,
        in_specs=[VMEM] * len(args),
        out_specs=[VMEM] * len(outs),
        scratch_shapes=[
            *scratch,
            pltpu.SemaphoreType.DMA((messages,)),
            pltpu.SemaphoreType.DMA((messages,)),
        ],
        compiler_params=pltpu.CompilerParams(
            collective_id=cid, has_side_effects=True, vmem_limit_bytes=limit
        ),
        name=body.__name__,
    )(*args)


def attend(blocks, scale, ql, qr, lat, rope, up, att, ml):
    i = pl.program_id(0)
    rows = ql.shape[0]
    keys = lat.shape[1]
    plane = blocks * rows
    s = jnp.dot(ql[...], lat[...], preferred_element_type=jnp.float32)
    s = s + jnp.dot(qr[...], rope[...], preferred_element_type=jnp.float32)
    z, y = lax.axis_index("z"), lax.axis_index("y")
    ny = lax.axis_size("y")
    per = plane // ny
    query_at = z * plane + lax.rem(i, blocks) * rows + lax.broadcasted_iota(jnp.int32, (rows, 1), 0)
    lane = lax.broadcasted_iota(jnp.int32, (1, keys), 1)
    key_at = (lane // per) * plane + y * per + lax.rem(lane, per)
    allowed = key_at <= query_at
    s = jnp.where(allowed, s * scale, masked_score)
    top = jnp.max(s, axis=1, keepdims=True)
    w = jnp.where(allowed, jnp.exp(s - top), 0.0)
    total = jnp.sum(w, axis=1, keepdims=True)
    mixed = lax.dot_general(
        w.astype(jnp.bfloat16), lat[...], (((1,), (1,)), ((), ())), preferred_element_type=jnp.float32
    )
    share = (mixed / jnp.maximum(total, 1e-30)).astype(jnp.bfloat16)
    att[...] = jnp.dot(share, up[...], preferred_element_type=jnp.float32).astype(jnp.bfloat16)
    side = lax.broadcasted_iota(jnp.int32, (rows, LANES), 1)
    ml[...] = jnp.where(side == 0, top, total).T[:8]


def attention_call(ql, qr, lat, rope, up, heads, plane):
    rows = min(256, plane)
    blocks = plane // rows
    scale = (PLAIN_QK_WIDTH + QK_ROPE) ** (-0.5)
    total, width = ql.shape
    v = up.shape[1] // heads
    flops = 2 * total * lat.shape[1] * (2 * width + qr.shape[1]) + 2 * total * width * v
    return pl.pallas_call(
        functools.partial(attend, blocks, scale),
        grid=(total // rows,),
        out_shape=[
            jax.ShapeDtypeStruct((total, v), jnp.bfloat16),
            jax.ShapeDtypeStruct((8, total), jnp.float32),
        ],
        in_specs=[
            pl.BlockSpec((rows, width), lambda i: (i, 0)),
            pl.BlockSpec((rows, qr.shape[1]), lambda i: (i, 0)),
            pl.BlockSpec(lat.shape, lambda i: (0, 0)),
            pl.BlockSpec(rope.shape, lambda i: (0, 0)),
            pl.BlockSpec((width, v), lambda i: (0, i // blocks)),
        ],
        out_specs=[
            pl.BlockSpec((rows, v), lambda i: (i, 0)),
            pl.BlockSpec((8, rows), lambda i: (0, i)),
        ],
        compiler_params=pltpu.CompilerParams(vmem_limit_bytes=32 * MIB),
        cost_estimate=pl.CostEstimate(
            flops=flops, bytes_accessed=6 * MIB, transcendentals=total * lat.shape[1]
        ),
        name="attend",
    )(ql, qr, lat, rope, up)


def angles_at(positions, indices, width):
    inverse = rope_base ** (-2.0 * indices.astype(jnp.float32) / width)
    return positions[:, None] * inverse[None, :]


def local(
    tokens,
    norm_gain,
    w_value,
    w_gate,
    conv_taps,
    conv_gain,
    w_query,
    latent_down_weight,
    latent_norm_gain,
    w_rope_key,
    key_up_weight,
    value_up_weight,
    w_merge_conv,
    w_merge_attn,
):
    bf16, f32 = jnp.bfloat16, jnp.float32
    sizes = nz, ny, nx, nc = tuple(lax.axis_size(a) for a in ("z", "y", "x", "c"))
    z, y, x, c = (lax.axis_index(a) for a in ("z", "y", "x", "c"))
    ntp = nx * nc
    j = x * nc + c
    rows, feats = tokens.shape
    width = feats * ntp
    plane = rows * ny
    wr, chans = w_value.shape
    share = chans // ny
    rank = latent_down_weight.shape[1]
    lat_share, rope_share = rank // ntp, QK_ROPE // ntp
    pairs = rope_share // 2
    kept = lat_share + rope_share
    middle = QK_ROPE // 2

    rope_cols = w_rope_key.reshape(wr, 2, ntp, pairs)
    rope_part = lax.dynamic_slice_in_dim(rope_cols, j, 1, 2).reshape(wr, rope_share)
    lat_part = lax.dynamic_slice_in_dim(latent_down_weight, j * lat_share, lat_share, 1)
    lw = jnp.concatenate([lat_part, rope_part, jnp.zeros((wr, LANES - kept), bf16)], axis=1)
    vg = jnp.concatenate(
        [w_value.reshape(wr, ny, share), w_gate.reshape(wr, ny, share)], axis=2
    ).transpose(1, 0, 2)

    messages = (3 + 2 * ny + 3 * nx) + 2 * ny + 4 * nx * ny + 20 + ny + nx
    X, WL, VG = kernel_call(
        gather_inputs,
        sizes,
        [
            jax.ShapeDtypeStruct((ny, rows, width), bf16),
            jax.ShapeDtypeStruct((kept, nz * LANES), bf16),
            jax.ShapeDtypeStruct((ny * wr, 2 * share), bf16),
        ],
        messages,
        0,
        (tokens, lw, vg),
        scratch=[pltpu.VMEM((ny, wr, LANES), bf16)],
    )
    features = X.reshape(plane, width).astype(f32)
    normed = (
        features
        * lax.rsqrt(jnp.mean(features * features, axis=-1, keepdims=True) + epsilon)
        * norm_gain
    ).astype(bf16)
    normed_own = lax.dynamic_slice_in_dim(normed, y * rows, rows, 0)

    pre = lax.dot_general(WL, normed_own, (((1,), (1,)), ((), ())), preferred_element_type=f32)
    first_row = (z * ny + y) * rows
    own_at = (first_row + jnp.arange(rows, dtype=jnp.int32)).astype(f32)
    own_angle = angles_at(own_at, j * pairs + jnp.arange(pairs, dtype=jnp.int32), QK_ROPE).T
    first, second = pre[lat_share : lat_share + pairs], pre[lat_share + pairs :]
    cosine, sine = jnp.cos(own_angle), jnp.sin(own_angle)
    own = jnp.concatenate(
        [pre[:lat_share], first * cosine - second * sine, first * sine + second * cosine], axis=0
    ).astype(bf16)

    K, W = kernel_call(
        gather_latent,
        sizes,
        [
            jax.ShapeDtypeStruct((ntp, kept, nz * rows), bf16),
            jax.ShapeDtypeStruct((nz * ny * wr, 2 * share), bf16),
        ],
        2 * 20 + nz * (2 * nx),
        1,
        (own, VG),
    )
    keys = nz * rows
    raw = K[:, :lat_share].reshape(rank, keys).astype(f32)
    latent = (
        raw
        * lax.rsqrt(jnp.mean(raw * raw, axis=0, keepdims=True) + epsilon)
        * latent_norm_gain[:, None]
    ).astype(bf16)
    key_rope = (
        K[:, lat_share:].reshape(ntp, 2, pairs, keys).transpose(1, 0, 2, 3).reshape(QK_ROPE, keys)
    )

    heads = key_up_weight.shape[1] // PLAIN_QK_WIDTH
    query = (
        jnp.dot(normed, w_query, preferred_element_type=f32)
        .astype(bf16)
        .reshape(plane, heads, PLAIN_QK_WIDTH + QK_ROPE)
    )
    plane_at = (z * plane + jnp.arange(plane, dtype=jnp.int32)).astype(f32)
    angle = angles_at(plane_at, jnp.arange(middle, dtype=jnp.int32), QK_ROPE)[:, None, :]
    turned = query[..., PLAIN_QK_WIDTH:].astype(f32)
    first, second = turned[..., :middle], turned[..., middle:]
    cosine, sine = jnp.cos(angle), jnp.sin(angle)
    query_rope = jnp.concatenate(
        [first * cosine - second * sine, first * sine + second * cosine], axis=-1
    ).astype(bf16)
    query_latent = jnp.einsum(
        "thd,lhd->htl",
        query[..., :PLAIN_QK_WIDTH],
        key_up_weight.reshape(rank, heads, PLAIN_QK_WIDTH),
        preferred_element_type=f32,
    ).astype(bf16)

    both = jnp.dot(normed, W, preferred_element_type=f32)
    gated = (both[:, :share] * jax.nn.sigmoid(both[:, share:])).astype(bf16)
    reach = conv_taps.shape[0] - 1
    prior = lax.ppermute(gated[plane - reach :], "z", [(i, i + 1) for i in range(nz - 1)])

    att, ml = attention_call(
        query_latent.reshape(heads * plane, rank),
        query_rope.transpose(1, 0, 2).reshape(heads * plane, QK_ROPE),
        latent,
        key_rope,
        value_up_weight,
        heads,
        plane,
    )

    taps = lax.dynamic_slice_in_dim(conv_taps, y * share, share, 1).astype(f32)
    padded = jnp.concatenate([prior, gated], axis=0).astype(f32)
    mixed = jnp.zeros(gated.shape, f32)
    for tap in range(reach + 1):
        mixed = mixed + taps[tap] * padded[tap : tap + plane]

    mid = rows // 2
    packed = jnp.concatenate(
        [mixed.reshape(ny, 2, mid, share)[:, 0], mixed.reshape(ny, 2, mid, share)[:, 1]], axis=2
    )
    tops = ml[0].reshape(heads, ny, rows)
    sums = ml[1].reshape(heads, ny, rows)
    stats = jnp.stack([jnp.sum(mixed, axis=1), jnp.sum(mixed * mixed, axis=1)]).reshape(2, ny, rows)
    st = jnp.concatenate([stats, tops, sums], axis=0).transpose(1, 0, 2)
    st = jnp.concatenate([st, jnp.zeros((ny, 8 - st.shape[1], rows), f32)], axis=1)
    att_r, mixed_r, st_r, stat_r = kernel_call(
        exchange,
        sizes,
        [
            jax.ShapeDtypeStruct((ny, heads, rows, VALUE_HEAD_WIDTH), bf16),
            jax.ShapeDtypeStruct((ny, mid, 2 * share), f32),
            jax.ShapeDtypeStruct((ny, 8, rows), f32),
            jax.ShapeDtypeStruct((ntp, 8, rows), f32),
        ],
        3 * ny + ntp,
        2,
        (att.reshape(heads, plane, VALUE_HEAD_WIDTH), packed, st),
    )
    tops, sums = st_r[:, 2 : 2 + heads], st_r[:, 2 + heads : 2 + 2 * heads]
    top = jnp.max(tops, axis=0)
    factor = jnp.exp(tops - top) * sums
    total = jnp.sum(factor, axis=0)
    log_sums = (top + jnp.log(total)).T
    factor = factor / total
    attention = (
        jnp.sum(factor[..., None] * att_r.astype(f32), axis=0)
        .astype(bf16)
        .transpose(1, 0, 2)
        .reshape(rows, heads * VALUE_HEAD_WIDTH)
    )
    channel_stats = jnp.sum(stat_r[:, :2], axis=0)
    channel_total = chans * ntp
    channel_mean = channel_stats[0] / channel_total
    channel_var = channel_stats[1] / channel_total - channel_mean * channel_mean
    own_mixed = (
        mixed_r.reshape(ny, mid, 2, share).transpose(2, 1, 0, 3).reshape(rows, chans)
    )
    conv_out = jax.nn.silu(
        (own_mixed - channel_mean[:, None]) * lax.rsqrt(channel_var + epsilon)[:, None] * conv_gain
    ).astype(bf16)
    part = (
        jnp.dot(conv_out, w_merge_conv, preferred_element_type=f32)
        + jnp.dot(attention, w_merge_attn, preferred_element_type=f32)
    ).astype(bf16)
    (parts,) = kernel_call(
        scatter_rows,
        sizes,
        [jax.ShapeDtypeStruct((ntp, rows // ntp, part.shape[1]), bf16)],
        ntp,
        3,
        (part.reshape(ntp, rows // ntp, part.shape[1]),),
    )
    merged = jnp.sum(parts.astype(f32), axis=0).astype(bf16)
    return merged, log_sums


def solution(mesh):
    devices = mesh.devices
    shape = (devices.shape[0] // 4, 4, 4, 2)
    finer = Mesh(devices.reshape(shape), ("z", "y", "x", "c"))
    return jax.shard_map(
        local,
        mesh=finer,
        in_specs=(
            P(SP, TP),
            P(),
            P(SP, TP),
            P(SP, TP),
            P(None, TP),
            P(TP),
            P(None, TP),
            P(SP, None),
            P(),
            P(SP, None),
            P(None, TP),
            P(None, TP),
            P(TP, None),
            P(TP, None),
        ),
        out_specs=(P((*SP, *TP), None), P(SP, TP)),
        check_vma=False,
    )
```

```python
import functools

import jax
import jax.numpy as jnp
import numpy as np
import numpy as np
import numpy as np
from jax import lax
from jax.experimental import pallas as pl
from jax.experimental.pallas import tpu as pltpu
from jax.sharding import Mesh
from jax.sharding import PartitionSpec as P

PLAIN_QK_WIDTH = 128
QK_ROPE = 64
VALUE_HEAD_WIDTH = 128
epsilon = 1e-06
rope_base = 10000.0
masked_score = -1e30
SP = ("z", "y")
TP = ("x", "c")
LANES = 128
VMEM = pl.BlockSpec(memory_space=pltpu.VMEM)
MIB = 1 << 20


class Net:
    def __init__(self, sizes, send, recv):
        self.nz, self.ny, self.nx, self.nc = sizes
        self.z, self.y, self.x, self.c = (lax.axis_index(a) for a in ("z", "y", "x", "c"))
        self.send, self.recv = send, recv
        self.ids, self.open = {}, []

    def number(self, name):
        return self.ids.setdefault(name, len(self.ids))

    def put(self, name, src, dst, **to):
        k = self.number(name)
        copy = pltpu.make_async_remote_copy(
            src_ref=src,
            dst_ref=dst,
            send_sem=self.send.at[k],
            recv_sem=self.recv.at[k],
            device_id=to,
            device_id_type=pl.DeviceIdType.MESH,
        )
        copy.start()
        self.open.append(copy)

    def got(self, name, dst, **to):
        k = self.number(name)
        pltpu.make_async_remote_copy(
            src_ref=dst,
            dst_ref=dst,
            send_sem=self.send.at[k],
            recv_sem=self.recv.at[k],
            device_id=to,
            device_id_type=pl.DeviceIdType.MESH,
        ).wait_recv()

    def finish(self):
        for copy in self.open:
            copy.wait_send()

    def zp(self, d):
        return lax.rem(self.z + d + self.nz, self.nz)

    def yp(self, d):
        return lax.rem(self.y + d + self.ny, self.ny)

    def xp(self, d):
        return lax.rem(self.x + d + self.nx, self.nx)

    def cp(self):
        return 1 - self.c

    def greet(self, peers):
        barrier = pltpu.get_barrier_semaphore()
        for to in peers:
            pl.semaphore_signal(barrier, inc=1, device_id=to, device_id_type=pl.DeviceIdType.MESH)
        pl.semaphore_wait(barrier, len(peers))


def z_plan(nz):
    group = 4 if nz >= 16 else 2
    count = nz // group
    if group == 4:
        near = {1: range(count), -1: range(count), 2: (0, 1), -2: (1, 2)}
    else:
        near = {1: range(count)}
    return group, count, near


def z_order(nz):
    group, count, near = z_plan(nz)
    order = [0] + [group * b for b in ((1, 3, 2) if count == 4 else range(1, count))]
    for b in (0, 1, 3, 2) if count == 4 else range(count):
        for d, blocks in near.items():
            if b in blocks:
                order.append((b * group - d) % nz)
    return order


def z_peers(net):
    group, count, near = z_plan(net.nz)
    far = (1, -1) if count > 2 else (1,) if count == 2 else ()
    peers = [{"z": net.zp(d)} for d in [group * f for f in far] + list(near)]
    if group == 2:
        peers.append({"z": net.zp(-1)})
    return peers


class ZGather:
    def __init__(self, net, tag, here, there):
        self.net, self.tag, self.here, self.there = net, tag, here, there
        self.group, self.count, self.near = z_plan(net.nz)
        z_class = net.z // self.group
        self.turn = jnp.where(lax.rem(z_class, 2) == 1, 1, -1)

    def start(self):
        n, g = self.net, self.group
        if self.count >= 2:
            n.put((self.tag, "f", 1), self.here(0), self.there(0, g), z=n.zp(g))
        if self.count > 2:
            n.put((self.tag, "f", -1), self.here(0), self.there(0, -g), z=n.zp(-g))
        self.spread(0)

    def spread(self, b):
        n = self.net
        k = b * self.group
        for d, blocks in self.near.items():
            if b in blocks:
                n.put((self.tag, "n", d, b), self.here(k), self.there(k, d), z=n.zp(d))

    def far_first(self):
        n, g = self.net, self.group
        if self.count == 2:
            n.got((self.tag, "f", 1), self.here(g), z=n.zp(g))
            self.spread(1)
            return [g]
        n.got((self.tag, "f", 1), self.here(3 * g), z=n.zp(g))
        n.got((self.tag, "f", -1), self.here(g), z=n.zp(g))
        n.put(
            (self.tag, "r"), self.here(-g * self.turn), self.there(-g * self.turn, g * self.turn),
            z=n.zp(g * self.turn),
        )
        self.spread(1)
        self.spread(3)
        return [g, 3 * g]

    def far_last(self):
        n, g = self.net, self.group
        if self.count == 2:
            return []
        n.got((self.tag, "r"), self.here(2 * g), z=n.zp(g))
        self.spread(2)
        return [2 * g]

    def close(self, picked=None):
        n, g = self.net, self.group
        for b in (0, 1, 3, 2) if self.count == 4 else range(self.count):
            for d, blocks in self.near.items():
                if b in blocks and (picked is None or b in picked):
                    at = (b * g - d) % n.nz
                    n.got((self.tag, "n", d, b), self.here(at), z=n.zp(d))
                    yield at


def tile(i, size):
    return pl.ds(pl.multiple_of(i * size, size), size)


def turned(v, shift):
    return pltpu.roll(v, shift, 1)


def layer(
    sizes, tok, wv, wg, wl, wr, gain, lgain, taps, cgain, invq, invk, wq_h, ku_h, vu_h, wc_h, wa_h,
    merged, logs,
    X, N, WL, VG, W, yb, lw, vg, wide, K, LA, QA, M, L, ACC, G, MX, ATT, CS, ML, LG,
    att_r, mix_r, cs_r, ml_r, stat_r, CP, PART, parts_r,
    wq, ku, vu, wc, wa, load, send, recv,
):
    f32, bf16 = jnp.float32, jnp.bfloat16
    net = Net(sizes, send, recv)
    nz, ny, nx, nc = sizes
    ntp = nx * nc
    z, y, x, c = net.z, net.y, net.x, net.c
    o = net.cp()
    j = x * nc + c
    rows, feats = tok.shape
    half = feats // 2
    width = X.shape[1]
    plane = rows * ny
    wrows = wv.shape[0]
    rank = lgain.shape[1]
    lat_share = rank // ntp
    rope_share = QK_ROPE // ntp
    pairs = rope_share // 2
    kept = lat_share + rope_share
    share = wv.shape[1] // ny
    heads = vu.shape[1] // VALUE_HEAD_WIDTH
    keys = nz * rows
    mid = rows // 2

    loads = []
    for k, (src, dst) in enumerate(((wq_h, wq), (ku_h, ku), (vu_h, vu), (wc_h, wc), (wa_h, wa))):
        loads.append(pltpu.make_async_copy(src, dst, load.at[k]))
        loads[-1].start()

    offsets = [(a, b) for a in range(nx) for b in range(nc) if a or b]

    def there(a, b):
        return {"x": net.xp(a), "c": c if b == 0 else o}

    peers = [{"y": net.yp(k)} for k in range(1, ny)] + [there(a, b) for a, b in offsets]
    peers += z_peers(net)
    barrier = pltpu.get_barrier_semaphore()
    for to in peers:
        pl.semaphore_signal(barrier, inc=1, device_id=to, device_id_type=pl.DeviceIdType.MESH)

    lane = lax.broadcasted_iota(jnp.int32, (wrows, LANES), 1)
    low = lane < share
    for t in range(ny):
        v = wv[:, t // 2 * LANES : (t // 2 + 1) * LANES].astype(f32)
        g = wg[:, t // 2 * LANES : (t // 2 + 1) * LANES].astype(f32)
        v, g = (v, turned(g, share)) if t % 2 == 0 else (turned(v, share), g)
        vg[t] = jnp.where(low, v, g).astype(bf16)
    lat = wl[:, tile(j // 2, LANES)].astype(f32)
    lat = jnp.where(lax.rem(j, 2) == 0, lat, turned(lat, lat_share))
    wide[...] = jnp.zeros(wide.shape, f32)
    wide[:, :QK_ROPE] = wr[...].astype(f32)
    rope = wide[...]
    rope_a = turned(rope, lat_share - pairs * j)
    rope_b = turned(rope, LANES + lat_share + pairs - QK_ROPE // 2 - pairs * j)
    lw[...] = jnp.where(
        lane < lat_share, lat, jnp.where(lane < lat_share + pairs, rope_a, rope_b)
    ).astype(bf16)
    yb[pl.ds(y, 1)] = lw[...][None]
    VG[tile(y, wrows)] = vg[pl.ds(y, 1)].reshape(vg.shape[1:])

    pl.semaphore_wait(barrier, len(peers))

    def cols(side, xx, cc):
        return tile((xx * nc + cc) * 2 + side, half)

    def place(side, yy, xx, cc):
        return X.at[tile(yy, rows), cols(side, xx, cc)]

    mine = [tok.at[:, pl.ds(0, half)], tok.at[:, pl.ds(half, half)]]
    for k in range(1, ny):
        net.put(("lw", k), lw, yb.at[y], y=net.yp(k))
    for k in range(1, ny):
        net.put(("ya", k), mine[0], place(0, y, x, c), y=net.yp(k))
    for k in range(1, nx):
        net.put(("xb", k), mine[1], place(1, y, x, c), x=net.xp(k))
    for k in range(1, nx):
        net.put(("xa", 0, k), mine[0], place(0, y, x, c), x=net.xp(k))
    for k in range(1, ny):
        net.put(("vg", k), vg.at[net.yp(k)], VG.at[tile(y, wrows)], y=net.yp(k))
    for k in range(1, ny):
        net.put(("yb", 0, k), mine[1], place(1, y, x, c), y=net.yp(k))
    for side in (0, 1):
        net.put(("s", side), mine[side], place(side, y, x, c), c=o)
        X[tile(y, rows), cols(side, x, c)] = tok[:, side * half : (side + 1) * half]

    for k in range(1, ny):
        net.got(("lw", k), yb.at[net.yp(-k)], y=net.yp(k))
    WL[:, tile(z, LANES)] = yb[...].reshape(ny * wrows, LANES).astype(f32).T[:kept].astype(bf16)
    zg = ZGather(
        net, "wl", lambda n: WL.at[:, tile(net.zp(n), LANES)],
        lambda n, d: WL.at[:, tile(net.zp(n), LANES)],
    )
    zg.start()

    for k in range(1, ny):
        at = place(0, net.yp(-k), x, c)
        net.got(("ya", k), at, y=net.yp(k))
        for i in range(1, nx):
            net.put(("xa", k, i), at, at, x=net.xp(i))
        net.put(("sa", k), at, at, c=o)
    for k in range(1, nx):
        at = place(1, y, net.xp(-k), c)
        net.got(("xb", k), at, x=net.xp(k))
        for i in range(1, ny):
            net.put(("yb", k, i), at, at, y=net.yp(i))
        net.put(("sb", k), at, at, c=o)
    for k in range(1, ny):
        net.got(("vg", k), VG.at[tile(net.yp(-k), wrows)], y=net.yp(k))
    depth = ny * wrows
    W[tile(z, depth)] = VG[...]
    zw = ZGather(
        net, "w", lambda n: W.at[tile(net.zp(n), depth)], lambda n, d: W.at[tile(net.zp(n), depth)]
    )
    zw.start()
    zg.far_first()
    for k in range(ny):
        for i in range(1, nx):
            at = place(0, net.yp(-k), net.xp(-i), c)
            net.got(("xa", k, i), at, x=net.xp(i))
            net.put(("sxa", k, i), at, at, c=o)
    for k in range(nx):
        for i in range(1, ny):
            at = place(1, net.yp(-i), net.xp(-k), c)
            net.got(("yb", k, i), at, y=net.yp(i))
            net.put(("syb", k, i), at, at, c=o)
    zw.far_first()
    zg.far_last()
    for side in (0, 1):
        net.got(("s", side), place(side, y, x, o), c=o)
    for k in range(1, ny):
        net.got(("sa", k), place(0, net.yp(-k), x, o), c=o)
    for k in range(1, nx):
        net.got(("sb", k), place(1, y, net.xp(-k), o), c=o)
    for k in range(ny):
        for i in range(1, nx):
            net.got(("sxa", k, i), place(0, net.yp(-k), net.xp(-i), o), c=o)
    for k in range(nx):
        for i in range(1, ny):
            net.got(("syb", k, i), place(1, net.yp(-i), net.xp(-k), o), c=o)

    piece = min(64, rows)

    def norm_rows(i, _):
        at = tile(i, piece)
        v = X[at, :].astype(f32)
        v = v * lax.rsqrt(jnp.mean(v * v, axis=1, keepdims=True) + epsilon) * gain[...]
        N[at, :] = v.astype(bf16)
        return _

    lax.fori_loop(0, plane // piece, norm_rows, 0)
    zw.far_last()

    loads[0].wait()
    loads[1].wait()
    band = min(128, plane)

    def query_rows(i, _):
        at = tile(i, band)
        q = jnp.dot(N[at, :], wq[...], preferred_element_type=f32).astype(bf16).astype(f32)
        lanes = lax.broadcasted_iota(jnp.int32, (band, LANES), 1)
        first_head = lanes < QK_ROPE
        b, d = q[:, LANES : 2 * LANES], q[:, 2 * LANES :]
        plain = (
            q[:, :LANES],
            jnp.where(first_head, turned(b, QK_ROPE), turned(d, QK_ROPE)),
        )
        rot = jnp.where(first_head, b, d)
        pos = z * plane + i * band + lax.broadcasted_iota(jnp.int32, (band, LANES), 0)
        ang = pos.astype(f32) * invq[...]
        front = lax.rem(lanes, QK_ROPE) < QK_ROPE // 2
        swap = jnp.where(front, turned(rot, LANES - QK_ROPE // 2), turned(rot, QK_ROPE // 2))
        sine = jnp.sin(ang)
        rot = rot * jnp.cos(ang) + swap * jnp.where(front, -sine, sine)
        for h in range(heads):
            ql = lax.dot_general(
                plain[h].astype(bf16), ku[:, h * LANES : (h + 1) * LANES],
                (((1,), (1,)), ((), ())), preferred_element_type=f32,
            )
            to = tile(h * (plane // band) + i, band)
            QA[to, :rank] = ql.astype(bf16)
            QA[to, rank:] = jnp.where(first_head == (h == 0), rot, 0.0).astype(bf16)
        return _

    lax.fori_loop(0, plane // band, query_rows, 0)
    for _ in zg.close():
        pass

    pre = lax.dot_general(
        WL[...], N[tile(y, rows), :], (((1,), (1,)), ((), ())), preferred_element_type=f32
    )
    angle = (
        (z * plane + y * rows + lax.broadcasted_iota(jnp.int32, (rope_share, rows), 1)).astype(f32)
        * invk[tile(j, rope_share), :rows]
    )
    part = pre[lat_share:]
    second = lax.broadcasted_iota(jnp.int32, (rope_share, rows), 0) >= pairs
    other = pltpu.roll(part, pairs, 0)
    part = part * jnp.cos(angle) + other * jnp.where(second, jnp.sin(angle), -jnp.sin(angle))

    order = z_order(nz)
    spot = {n: k for k, n in enumerate(order)}

    def slot(n, jj=None):
        if isinstance(n, int):
            at = pl.ds(spot[n % nz] * rows, rows)
        else:
            g = z_plan(nz)[0]
            at = tile(jnp.where(n > 0, spot[g], spot[nz - g]), rows)
        return K.at[j if jj is None else jj, :, at]

    def slot_there(n, d):
        if isinstance(n, int):
            return slot(n - d)
        return slot(2 * z_plan(nz)[0])

    K[pl.ds(j, 1), :lat_share, :rows] = pre[:lat_share].astype(bf16)[None]
    K[pl.ds(j, 1), lat_share:, :rows] = part.astype(bf16)[None]
    zl = ZGather(net, "l", slot, slot_there)

    def onward(n):
        for k in range(1, nx):
            net.put(("x", n, k), slot(n), slot(n), x=net.xp(k))
        net.put(("ls", n), slot(n), slot(n), c=o)

    zl.start()
    onward(0)
    LG[...] = jnp.broadcast_to(lgain[...], (rows, rank)).T
    for _ in zw.close():
        pass
    @pl.when(z == 0)
    def _():
        G[:32] = jnp.zeros((32, LANES), f32)

    def gated_rows(i, _):
        both = jnp.dot(N[tile(i, band), :], W[...], preferred_element_type=f32)
        gate = turned(both, share)
        g = both * jax.nn.sigmoid(gate)
        G[pl.ds(pl.multiple_of(32 + i * band, 8), band), :] = g.astype(bf16).astype(f32)
        return _

    lax.fori_loop(0, plane // band, gated_rows, 0)
    @pl.when(z < nz - 1)
    def _():
        k = net.number(("halo",))
        pltpu.make_async_remote_copy(
            src_ref=G.at[pl.ds(plane, 32)], dst_ref=G.at[pl.ds(0, 32)],
            send_sem=send.at[k], recv_sem=recv.at[k],
            device_id={"z": net.zp(1)}, device_id_type=pl.DeviceIdType.MESH,
        ).start()

    def arrive(ns):
        for n in ns:
            for k in range(1, nx):
                at = slot(n, net.xp(-k) * nc + c)
                net.got(("x", n, k), at, x=net.xp(k))
                net.put(("sx", n, k), at, at, c=o)

    def sibling(ns):
        for n in ns:
            net.got(("ls", n), slot(n, x * nc + o), c=o)
            for k in range(1, nx):
                net.got(("sx", n, k), slot(n, net.xp(-k) * nc + o), c=o)

    def keys_of(first, count):
        for s in range(first, first + count):
            at = pl.ds(s * rows, rows)
            raw = [K[t, :lat_share, at].astype(f32) for t in range(ntp)]
            total = sum(jnp.sum(r * r, axis=0, keepdims=True) for r in raw)
            scale = lax.rsqrt(total / rank + epsilon)
            for t in range(ntp):
                span = slice(t * lat_share, (t + 1) * lat_share)
                LA[span, at] = (raw[t] * scale * LG[span]).astype(bf16)
            r = [K[t, lat_share:, at].astype(f32) for t in range(ntp)]
            if pairs == 4:
                upper = lax.broadcasted_iota(jnp.int32, (8, rows), 0) < 4
                lo = [
                    jnp.where(upper, r[t], pltpu.roll(r[t + 1], 4, 0)) for t in range(0, ntp, 2)
                ]
                hi = [
                    jnp.where(upper, pltpu.roll(r[t], 4, 0), r[t + 1]) for t in range(0, ntp, 2)
                ]
            else:
                lo, hi = [v[:pairs] for v in r], [v[pairs:] for v in r]
            rot = jnp.concatenate(lo + hi, axis=0).astype(bf16)
            LA[rank : rank + QK_ROPE, at] = rot
            LA[rank + QK_ROPE :, at] = rot

    score_scale = (PLAIN_QK_WIDTH + QK_ROPE) ** (-0.5)

    def attend(first, count, h, fresh):
        at = pl.ds(first * rows, count * rows)
        to = pl.ds(h * plane, plane)
        lanes = lax.broadcasted_iota(jnp.int32, (1, count * rows), 1)
        key_at = jnp.zeros((1, count * rows), jnp.int32)
        for s in range(count):
            base = net.zp(order[first + s]) * plane + y * rows - s * rows
            key_at = jnp.where(lanes >= s * rows, base + lanes, key_at)
        query_at = z * plane + lax.broadcasted_iota(jnp.int32, (plane, 1), 0)
        s = jnp.dot(QA[to, :], LA[:, at], preferred_element_type=f32)
        s = jnp.where(key_at <= query_at, s * score_scale, masked_score)
        top = jnp.max(s, axis=1, keepdims=True)
        old = masked_score * 0.1 if fresh else M[to, :1]
        top = jnp.maximum(old, top)
        w = jnp.exp(s - top)
        total = jnp.sum(w, axis=1, keepdims=True)
        part = lax.dot_general(
            w.astype(bf16), LA[:rank, at], (((1,), (1,)), ((), ())), preferred_element_type=f32
        )
        if fresh:
            L[to, :] = jnp.broadcast_to(total, (plane, LANES))
            ACC[to, :] = part
        else:
            keep = jnp.exp(old - top)
            L[to, :] = L[to, :] * keep + total
            ACC[to, :] = ACC[to, :] * keep + part
        M[to, :] = jnp.broadcast_to(top, (plane, LANES))

    early, late = order[: max(1, nz // 4)], order[max(1, nz // 4) :]
    for n in zl.far_first():
        onward(n)

    @pl.when(z > 0)
    def _():
        k = net.number(("halo",))
        pltpu.make_async_remote_copy(
            src_ref=G.at[pl.ds(0, 32)], dst_ref=G.at[pl.ds(0, 32)],
            send_sem=send.at[k], recv_sem=recv.at[k],
            device_id={"z": net.zp(1)}, device_id_type=pl.DeviceIdType.MESH,
        ).wait_recv()

    reach = taps.shape[0] - 1
    t = taps[:, tile(y // 2, LANES)].astype(f32)
    low = lax.broadcasted_iota(jnp.int32, t.shape, 1) < share
    t = jnp.where(low == (lax.rem(y, 2) == 0), t, turned(t, share))
    low = lax.broadcasted_iota(jnp.int32, (mid, LANES), 1) < share
    for t_y in range(ny):
        lo = G[pl.ds(t_y * rows, mid + 32), :]
        hi = turned(G[pl.ds(t_y * rows + mid, mid + 32), :], share)
        wide = lax.broadcasted_iota(jnp.int32, (mid + 32, LANES), 1) < share
        both = jnp.where(wide, lo, hi)
        mixed = jnp.zeros((mid, LANES), f32)
        for k in range(reach + 1):
            off = 32 - reach + k
            mixed = mixed + t[k : k + 1] * both[off : off + mid]
        MX[t_y] = mixed
        spread = lax.broadcasted_iota(jnp.int32, (rows, LANES), 1)
        cs = jnp.zeros((rows, LANES), f32)
        for r, v in enumerate((mixed, mixed * mixed)):
            v = jnp.concatenate(
                [
                    jnp.sum(jnp.where(low, v, 0.0), axis=1, keepdims=True),
                    jnp.sum(jnp.where(low, 0.0, v), axis=1, keepdims=True),
                ],
                axis=0,
            )
            cs = jnp.where(spread == r, v, cs)
        CS[t_y] = cs.T[:8]
    for k in range(1, ny):
        to = net.yp(k)
        net.put(("cs", k), CS.at[to], cs_r.at[y], y=to)
    for k in range(1, ny):
        to = net.yp(k)
        net.put(("m", k), MX.at[to], mix_r.at[y], y=to)
    mix_r[pl.ds(y, 1)] = MX[pl.ds(y, 1)]
    cs_r[pl.ds(y, 1)] = CS[pl.ds(y, 1)]

    for n in zl.far_last():
        onward(n)
    for n in zl.close():
        onward(n)

    arrive(early)
    sibling(early)
    keys_of(0, len(early))
    for h in range(heads):
        attend(0, len(early), h, True)

    for k in range(1, ny):
        net.got(("cs", k), cs_r.at[net.yp(-k)], y=net.yp(k))
    stat_r[pl.ds(j, 1)] = sum(cs_r[k] for k in range(ny))[None]
    for a, b in offsets:
        net.put(("t", a, b), stat_r.at[j], stat_r.at[j], **there(a, b))
    for k in range(len(late)):
        arrive(late[k : k + 1])
        if k:
            sibling(late[k - 1 : k])
            keys_of(len(early) + k - 1, 1)

    def column(r):
        return jnp.broadcast_to(r, (LANES, rows)).T

    for k in range(1, ny):
        net.got(("m", k), mix_r.at[net.yp(-k)], y=net.yp(k))
    for a, b in offsets:
        jj = net.xp(-a) * nc + (c if b == 0 else o)
        net.got(("t", a, b), stat_r.at[jj], **there(a, b))
    stats = sum(stat_r[k] for k in range(ntp))
    channels = share * ny * ntp
    mean = stats[0:1] / channels
    var = stats[1:2] / channels - mean * mean
    mean, inv = column(mean), column(lax.rsqrt(var + epsilon))
    pieces = []
    for p in range(ny // 2):
        m0, m1 = mix_r[2 * p], mix_r[2 * p + 1]
        v = jnp.concatenate(
            [jnp.where(low, m0, turned(m1, share)), jnp.where(low, turned(m0, share), m1)], axis=0
        )
        v = (v - mean) * inv * cgain[:, p * LANES : (p + 1) * LANES]
        pieces.append((v * jax.nn.sigmoid(v)).astype(bf16))
    conv_out = jnp.concatenate(pieces, axis=1)
    for k in range(2, 5):
        loads[k].wait()
    cut = min(512, width)
    for k in range(width // cut):
        at = slice(k * cut, (k + 1) * cut)
        CP[:, at] = jnp.dot(conv_out, wc[:, at], preferred_element_type=f32)
    sibling(late[-1:])
    keys_of(nz - 1, 1)

    spread = lax.broadcasted_iota(jnp.int32, (rows, LANES), 1)
    for h in range(heads):
        attend(len(early), len(late), h, False)
        span = pl.ds(h * plane, plane)
        for t_y in range(ny):
            at = pl.ds(h * plane + t_y * rows, rows)
            ML[h, t_y] = jnp.where(spread == 0, M[at, :], L[at, :]).T[:8]
        for k in range(1, ny):
            to = net.yp(k)
            net.put(("ml", k, h), ML.at[h, to], ml_r.at[h, y], y=to)
        mean = (ACC[span, :] / jnp.maximum(L[span, :1], 1e-30)).astype(bf16)
        ATT[span, :] = jnp.dot(
            mean, vu[:, h * VALUE_HEAD_WIDTH : (h + 1) * VALUE_HEAD_WIDTH],
            preferred_element_type=f32,
        ).astype(bf16)
        for k in range(1, ny):
            to = net.yp(k)
            net.put(("a", k, h), ATT.at[tile(h * ny + to, rows), :], att_r.at[y, h], y=to)
        att_r[pl.ds(y, 1), h] = ATT[tile(h * ny + y, rows), :][None]
        ml_r[h, pl.ds(y, 1)] = ML[h, pl.ds(y, 1)]

    out, log_rows = [], []
    for h in range(heads):
        for k in range(1, ny):
            net.got(("ml", k, h), ml_r.at[h, net.yp(-k)], y=net.yp(k))
        tops = [ml_r[h, k, 0:1] for k in range(ny)]
        top = functools.reduce(jnp.maximum, tops)
        f = [jnp.exp(tops[k] - top) * ml_r[h, k, 1:2] for k in range(ny)]
        total = sum(f)
        log_rows.append(top + jnp.log(total))
        f = [column(v / total) for v in f]
        for k in range(1, ny):
            net.got(("a", k, h), att_r.at[net.yp(-k), h], y=net.yp(k))
        out.append(sum(f[k] * att_r[k, h].astype(f32) for k in range(ny)).astype(bf16))
    attention = jnp.concatenate(out, axis=1)
    logs[...] = jnp.concatenate(log_rows, axis=0)
    final = rows // ntp
    for k in range(width // cut):
        at = slice(k * cut, (k + 1) * cut)
        part = CP[:, at] + jnp.dot(attention, wa[:, at], preferred_element_type=f32)
        PART[:, at] = part.astype(bf16)
    for a, b in offsets:
        to = there(a, b)
        net.put(("p", a, b), PART.at[tile(to["x"] * nc + to["c"], final), :], parts_r.at[j], **to)
    total = PART[tile(j, final), :].astype(f32)
    for a, b in sorted(offsets, key=lambda v: min(v[0], nx - v[0])):
        source = there(-a, b)
        jj = source["x"] * nc + source["c"]
        net.got(("p", a, b), parts_r.at[jj], **there(a, b))
        total = total + parts_r[jj].astype(f32)
    merged[...] = total.astype(bf16)
    net.finish()

    @pl.when(z < nz - 1)
    def _():
        k = net.number(("halo",))
        pltpu.make_async_remote_copy(
            src_ref=G.at[pl.ds(plane, 32)], dst_ref=G.at[pl.ds(0, 32)],
            send_sem=send.at[k], recv_sem=recv.at[k],
            device_id={"z": net.zp(1)}, device_id_type=pl.DeviceIdType.MESH,
        ).wait_send()


def hand_on(a, b, a_out, b_out):
    a_out[...] = a[...]
    b_out[...] = b[...]


def local(
    tokens,
    norm_gain,
    w_value,
    w_gate,
    conv_taps,
    conv_gain,
    w_query,
    latent_down_weight,
    latent_norm_gain,
    w_rope_key,
    key_up_weight,
    value_up_weight,
    w_merge_conv,
    w_merge_attn,
):
    bf16, f32 = jnp.bfloat16, jnp.float32
    sizes = nz, ny, nx, nc = tuple(lax.axis_size(a) for a in ("z", "y", "x", "c"))
    ntp = nx * nc
    rows, feats = tokens.shape
    width = feats * ntp
    plane, keys = rows * ny, rows * nz
    wrows, chans = w_value.shape
    rank = latent_down_weight.shape[1]
    pairs = QK_ROPE // ntp // 2
    kept = rank // ntp + 2 * pairs
    heads = key_up_weight.shape[1] // PLAIN_QK_WIDTH
    mid = rows // 2
    middle = QK_ROPE // 2

    rates = np.float32(rope_base) ** (-2.0 * np.arange(middle, dtype=np.float32) / QK_ROPE)
    rates = rates.astype(np.float32)
    invq = jnp.asarray(np.tile(rates, LANES // middle)[None])
    by_row = [rates[t * pairs + i % pairs] for t in range(ntp) for i in range(2 * pairs)]
    invk = jnp.asarray(np.repeat(np.array(by_row, np.float32)[:, None], LANES, axis=1))

    args = (
        tokens, w_value, w_gate, latent_down_weight, w_rope_key, norm_gain[None], latent_norm_gain[None],
        conv_taps, conv_gain[None], invq, invk,
        w_query, key_up_weight, value_up_weight, w_merge_conv, w_merge_attn,
    )
    anywhere = pl.BlockSpec(memory_space=pl.ANY)
    messages = 400
    vm = pltpu.VMEM
    total = heads * plane
    scratch = [
        vm((plane, width), bf16),
        vm((plane, width), bf16),
        vm((kept, nz * LANES), bf16),
        vm((ny * wrows, LANES), bf16),
        vm((nz * ny * wrows, LANES), bf16),
        vm((ny, wrows, LANES), bf16),
        vm((wrows, LANES), bf16),
        vm((ny, wrows, LANES), bf16),
        vm((wrows, LANES), f32),
        vm((ntp, kept, keys), bf16),
        vm((rank + LANES, keys), bf16),
        vm((total, rank + LANES), bf16),
        vm((total, LANES), f32),
        vm((total, LANES), f32),
        vm((total, rank), f32),
        vm((plane + 32, LANES), f32),
        vm((ny, mid, LANES), f32),
        vm((total, VALUE_HEAD_WIDTH), bf16),
        vm((ny, 8, rows), f32),
        vm((heads, ny, 8, rows), f32),
        vm((rank, rows), f32),
        vm((ny, heads, rows, VALUE_HEAD_WIDTH), bf16),
        vm((ny, mid, LANES), f32),
        vm((ny, 8, rows), f32),
        vm((heads, ny, 8, rows), f32),
        vm((ntp, 8, rows), f32),
        vm((rows, width), f32),
        vm((rows, width), bf16),
        vm((ntp, rows // ntp, width), bf16),
        vm(w_query.shape, bf16),
        vm(key_up_weight.shape, bf16),
        vm(value_up_weight.shape, bf16),
        vm(w_merge_conv.shape, bf16),
        vm(w_merge_attn.shape, bf16),
        pltpu.SemaphoreType.DMA((5,)),
        pltpu.SemaphoreType.DMA((messages,)),
        pltpu.SemaphoreType.DMA((messages,)),
    ]
    result = pl.pallas_call(
        functools.partial(layer, sizes),
        out_shape=[
            jax.ShapeDtypeStruct((rows // ntp, width), bf16),
            jax.ShapeDtypeStruct((heads, rows), f32),
        ],
        in_specs=[VMEM] * 11 + [anywhere] * 5,
        out_specs=[VMEM, VMEM],
        scratch_shapes=scratch,
        compiler_params=pltpu.CompilerParams(
            collective_id=0, has_side_effects=True, vmem_limit_bytes=56 * MIB
        ),
        name="layer",
    )(*args)
    merged, logs = (
        pl.pallas_call(
            hand_on,
            out_shape=[jax.ShapeDtypeStruct(r.shape, r.dtype) for r in result],
            in_specs=[VMEM, VMEM],
            out_specs=[VMEM, VMEM],
            compiler_params=pltpu.CompilerParams(vmem_limit_bytes=MIB),
            name="hand_on",
        )(*result)
    )
    return merged, logs.T


def solution(mesh):
    devices = mesh.devices
    shape = (devices.shape[0] // 4, 4, 4, 2)
    finer = Mesh(devices.reshape(shape), ("z", "y", "x", "c"))
    return jax.shard_map(
        local,
        mesh=finer,
        in_specs=(
            P(SP, TP),
            P(),
            P(SP, TP),
            P(SP, TP),
            P(None, TP),
            P(TP),
            P(None, TP),
            P(SP, None),
            P(),
            P(SP, None),
            P(None, TP),
            P(None, TP),
            P(TP, None),
            P(TP, None),
        ),
        out_specs=(P((*SP, *TP), None), P(SP, TP)),
        check_vma=False,
    )
```
